32 devices in a mesh: rep: 4 (over z), fs: 4 (over y, x), tp: 2 (over core).
Axes of the slice: x: 2, y: 2, z: 4, core: 2. Of those that a mesh axis runs over, the one named last changes fastest.
Arguments:
- hidden_pre: bfloat16 [8192, 4096], P(('rep', 'fs'), 'tp'), may hold values from -6 to 6
- out_grad: bfloat16 [8192, 2048], P(('rep', 'fs')), may hold values from -8 to 8
- down_weight: bfloat16 [2048, 4096], P('fs', 'tp'), may hold values from -0.09375 to 0.09375
Outputs:
- hidden_grad: bfloat16 [8192, 4096], P(('rep', 'fs'), 'tp')
- weight_grad: float32 [2048, 4096], P('fs', 'tp')
The draws below stay inside these ranges and needn't reach their ends.
All inputs are finite; a program needn't handle non-finite values.
Results may differ from the reference program's by a relative error of at most 0.0049.
Values may be sent and summed in bfloat16 or wider, within the bound.
A program may use at most 64 MiB of HBM per device.

```python
import jax
import jax.numpy as jnp
from jax import lax

D = 2048
FF = 4096
TOK_DEV = 512
TOKENS = 8192


def strengthened(array, key, source, target, shards_of, factor):
    def block_of(axis_at):
        return (jnp.arange(array.shape[axis_at]) // (array.shape[axis_at] // shards_of)).reshape((-1,) + (1,) * (array.ndim - 1 - axis_at))

    one_side = jax.random.permutation(key, shards_of)[block_of(target)]
    far = (block_of(target) + shards_of // 2) % shards_of
    return jnp.where((block_of(source) == one_side) | (block_of(source) == far), factor * array, array)


def level_of(key, dims, split, low, largest):
    def one(axis_at, parts):
        draws = jax.random.uniform(jax.random.fold_in(jax.random.fold_in(key, 6), axis_at), (parts,), jnp.float32, low / len(split), largest / len(split))
        return jnp.repeat(jnp.exp(draws), dims[axis_at] // parts).reshape((-1,) + (1,) * (len(dims) - axis_at - 1))

    level = one(*split[0])
    for cut in split[1:]:
        level = level * one(*cut)
    return level


def bell_draw(stream_key, shape, deviation, most, split=(), held_as=jnp.bfloat16):
    entries = deviation * jax.random.normal(stream_key, shape, jnp.float32)
    if split:
        entries = entries * level_of(stream_key, shape, split, -0.22, 0.18)
    return jnp.clip(entries, -most, most).astype(held_as)


def gaussian_with(key, dims, scale, limit, shards, heavy, held_as=jnp.bfloat16):
    result = scale * jax.random.normal(key, dims, jnp.float32)
    if shards:
        result = result * level_of(key, dims, shards, -0.22, 0.18)
    return jnp.clip(strengthened(result, jax.random.fold_in(key, 3), *heavy), -limit, limit).astype(held_as)


def setup_inputs(seed: int = 0) -> dict:
    key_list = jax.random.split(jax.random.key(seed), 4)
    hidden_pre = bell_draw(key_list[0], (TOKENS, FF), 1.0, 6.0, ((0, 16), (1, 2)))
    out_grad = gaussian_with(key_list[1], (TOKENS, D), 1.0, 8.0, ((0, 16),), (0, 1, 16, 2.0))
    down_weight = bell_draw(key_list[2], (D, FF), FF ** -0.5, 0.09375, ((0, 4), (1, 2)))
    return dict(hidden_pre=hidden_pre, out_grad=out_grad, down_weight=down_weight)


def reference(hidden_pre, out_grad, down_weight):
    count = TOKENS // TOK_DEV
    pre_blocks = hidden_pre.reshape(count, TOK_DEV, FF)
    grad_blocks = out_grad.reshape(count, TOK_DEV, D)

    def one_block(total, inputs):
        pre_rows, grad_rows = inputs
        positive = jnp.maximum(pre_rows.astype(jnp.float32), jnp.float32(0.0))
        back = jnp.dot(grad_rows, down_weight, preferred_element_type=jnp.float32)
        hidden_rows = (2.0 * positive * back).astype(jnp.bfloat16)
        act = (positive * positive).astype(jnp.bfloat16)
        part = lax.dot_general(grad_rows, act, (((0,), (0,)), ((), ())), preferred_element_type=jnp.float32)
        part = part.astype(jnp.bfloat16)
        return total + part.astype(jnp.float32), hidden_rows

    start = jnp.zeros((D, FF), jnp.float32)
    total, hidden_rows = lax.scan(one_block, start, (pre_blocks, grad_blocks))
    hidden_grad = hidden_rows.reshape(TOKENS, FF)
    weight_grad = total * jnp.float32(TOKENS ** -0.5)
    return hidden_grad, weight_grad
```

```python
import functools
import math

import jax
import jax.numpy as jnp
from jax import lax
from jax.experimental import pallas as pl
from jax.experimental.pallas import tpu as pltpu
from jax.sharding import PartitionSpec as P

MESH = pl.DeviceIdType.MESH
BF = jnp.bfloat16
F32 = jnp.float32


def plain_body(hidden_pre, out_grad, down_weight):
    rows = hidden_pre.shape[0]
    ff_local = hidden_pre.shape[1]
    back = jnp.dot(
        out_grad,
        lax.all_gather(down_weight, "fs", axis=0, tiled=True),
        preferred_element_type=F32,
    )
    positive = jnp.maximum(hidden_pre.astype(F32), 0.0)
    hidden_grad = (2.0 * positive * back).astype(BF)
    act = (positive * positive).astype(BF)
    partial_value = lax.dot_general(
        out_grad, act, (((0,), (0,)), ((), ())), preferred_element_type=F32
    )
    partial_value = partial_value.astype(BF)
    received = lax.all_to_all(partial_value, "fs", split_axis=0, concat_axis=0, tiled=True)
    groups = lax.axis_size("fs")
    local_sum = jnp.sum(
        received.reshape(groups, received.shape[0] // groups, ff_local), axis=0, dtype=F32
    )
    total = lax.psum(local_sum, "rep")
    tokens_all = rows * lax.axis_size("rep") * groups
    return (hidden_grad, total * (1.0 / math.sqrt(tokens_all)))


def kernel(chunks, hp, og, w, hg_out, tot_out,
           ogcat, ogt, whalf, hpc, pbs, pbr, pbo, gs, gr, gown, zs, z1r, z2r, zt, hg,
           l_og, l_w, l_hp, o_hg, o_t,
           og_s, og_r, od_s, od_r, w_s, w_r, hp_s, hp_r, pb_s, pb_r, g_s, g_r,
           z1_s, z1_rs, z2_s, z2_rs, z3_s, z3_rs):
    rows, ff = hp.shape
    depth = w.shape[0]
    half = 2 * depth
    fc = ff // chunks
    part = rows // 2
    fs = lax.axis_index("fs")
    core = lax.axis_index("tp")
    z = lax.axis_index("rep")
    last = lax.axis_size("rep") - 1
    a, b = fs // 2, fs % 2
    apeer = {"fs": (1 - a) * 2 + b}
    bpeer = {"fs": a * 2 + (1 - b)}
    cpeer = {"tp": 1 - core}
    znext = {"rep": z + 1 - 2 * (z % 2)}
    zmid = {"rep": last - z}
    outer = jnp.logical_or(z == 0, z == last)
    inner = jnp.logical_not(outer)

    def remote(src, dst, ssem, rsem, peer):
        return pltpu.make_async_remote_copy(
            src_ref=src, dst_ref=dst, send_sem=ssem, recv_sem=rsem,
            device_id=peer, device_id_type=MESH)

    def cols(c):
        return pl.ds(pl.multiple_of(c * fc, fc), fc)

    mine = pl.ds(pl.multiple_of(b * depth, depth), depth)
    theirs = pl.ds(pl.multiple_of((1 - b) * depth, depth), depth)
    low = pl.ds(pl.multiple_of(core * part, part), part)
    mid = pl.ds(pl.multiple_of(rows + core * part, part), part)
    mid_other = pl.ds(pl.multiple_of(rows + (1 - core) * part, part), part)

    def load_og():
        return pltpu.make_async_copy(
            og.at[:, pl.ds(pl.multiple_of(a * half, half), half)], ogcat.at[pl.ds(0, rows)], l_og)

    def load_w(c):
        return pltpu.make_async_copy(w.at[:, cols(c)], whalf.at[c, mine], l_w.at[c])

    def load_hp(c):
        return pltpu.make_async_copy(hp.at[:, cols(c)], hpc.at[0, c], l_hp.at[c])

    def store_hg(c):
        return pltpu.make_async_copy(hg.at[c], hg_out.at[:, cols(c)], o_hg.at[c])

    def store_tot(c):
        return pltpu.make_async_copy(zt.at[c], tot_out.at[:, cols(c)], o_t.at[c])

    def send_og():
        return remote(og.at[low, pl.ds(pl.multiple_of((1 - a) * half, half), half)],
                      ogcat.at[mid], og_s, og_r, apeer)

    def send_od():
        return remote(ogcat.at[mid], ogcat.at[mid], od_s, od_r, cpeer)

    def recv_od():
        return remote(ogcat.at[mid_other], ogcat.at[mid_other], od_s, od_r, cpeer)

    def send_w(c):
        return remote(w.at[:, cols(c)], whalf.at[c, mine], w_s.at[c], w_r.at[c], bpeer)

    def recv_w(c):
        return remote(w.at[:, cols(c)], whalf.at[c, theirs], w_s.at[c], w_r.at[c], bpeer)

    def send_hp(c):
        return remote(hp.at[:, cols(c)], hpc.at[1, c], hp_s.at[c], hp_r.at[c], apeer)

    def send_pb(c):
        return remote(pbs.at[c], pbr.at[c], pb_s.at[c], pb_r.at[c], apeer)

    def send_g(c):
        return remote(gs.at[c], gr.at[c], g_s.at[c], g_r.at[c], bpeer)

    def send_z1(c):
        return remote(zs.at[c], z1r.at[c], z1_s.at[c], z1_rs.at[c], znext)

    def send_z2(c):
        return remote(zs.at[c], z2r.at[c], z2_s.at[c], z2_rs.at[c], zmid)

    def send_z3(c):
        return remote(zt.at[c], zt.at[c], z3_s.at[c], z3_rs.at[c], znext)

    barrier = pltpu.get_barrier_semaphore()
    for peer in (apeer, bpeer, cpeer, znext, zmid):
        pl.semaphore_signal(barrier, inc=1, device_id=peer, device_id_type=MESH)
    load_og().start()
    pl.semaphore_wait(barrier, 5)

    send_og().start()

    @pl.loop(0, chunks)
    def _(c):
        send_w(c).start()
        send_hp(c).start()
        load_w(c).start()
        load_hp(c).start()

    load_og().wait()
    ogt[:, 0:rows] = ogcat[0:rows, :].T
    send_og().wait_recv()
    send_od().start()
    recv_od().wait_recv()
    ogt[:, rows:2 * rows] = ogcat[rows:2 * rows, :].T

    @pl.loop(0, chunks)
    def _(c):
        load_w(c).wait()
        recv_w(c).wait_recv()
        pbs[c] = jnp.dot(ogcat[rows:2 * rows, :], whalf[c], preferred_element_type=F32).astype(BF)
        send_pb(c).start()
        pbo[c] = jnp.dot(ogcat[0:rows, :], whalf[c], preferred_element_type=F32)
        load_hp(c).wait()
        send_hp(c).wait_recv()
        positive = jnp.maximum(hpc[:, c].reshape(2 * rows, fc).astype(F32), 0.0)
        act = (positive * positive).astype(BF)
        gs[c] = jnp.dot(ogt[theirs, :], act, preferred_element_type=F32).astype(BF)
        send_g(c).start()
        gown[c] = jnp.dot(ogt[mine, :], act, preferred_element_type=F32)

    @pl.loop(0, chunks + 4)
    def _(i):
        @pl.when(i < chunks)
        def _():
            send_g(i).wait_recv()

            @pl.when(outer)
            def _():
                zs[i] = (gown[i] + gr[i].astype(F32)).astype(BF)
                send_z1(i).start()

        @pl.when(jnp.logical_and(inner, jnp.logical_and(i >= 1, i < chunks + 1)))
        def _():
            c = i - 1
            send_z1(c).wait_recv()
            zs[c] = (gown[c] + gr[c].astype(F32) + z1r[c].astype(F32)).astype(BF)
            send_z2(c).start()

        @pl.when(jnp.logical_and(inner, jnp.logical_and(i >= 2, i < chunks + 2)))
        def _():
            c = i - 2
            send_z2(c).wait_recv()
            zt[c] = (zs[c].astype(F32) + z2r[c].astype(F32)).astype(BF)
            send_z3(c).start()
            store_tot(c).start()

        @pl.when(jnp.logical_and(i >= 3, i < chunks + 3))
        def _():
            c = i - 3
            send_pb(c).wait_recv()
            positive = jnp.maximum(hpc[0, c].astype(F32), 0.0)
            hg[c] = (2.0 * positive * (pbo[c] + pbr[c].astype(F32))).astype(BF)
            store_hg(c).start()

        @pl.when(jnp.logical_and(outer, i >= 4))
        def _():
            c = i - 4
            send_z3(c).wait_recv()
            store_tot(c).start()

    send_og().wait_send()
    send_od().wait_send()

    @pl.loop(0, chunks)
    def _(c):
        send_w(c).wait_send()
        send_hp(c).wait_send()
        send_pb(c).wait_send()
        send_g(c).wait_send()
        store_hg(c).wait()
        store_tot(c).wait()

        @pl.when(outer)
        def _():
            send_z1(c).wait_send()

        @pl.when(inner)
        def _():
            send_z2(c).wait_send()
            send_z3(c).wait_send()


def paired_body(hidden_pre, out_grad, down_weight):
    rows, ff = hidden_pre.shape
    depth = down_weight.shape[0]
    chunks = max(1, ff // 256)
    fc = ff // chunks
    any_spec = pl.BlockSpec(memory_space=pl.ANY)

    def block(r, dtype):
        return pltpu.VMEM((chunks, r, fc), dtype)

    sem = pltpu.SemaphoreType.DMA
    hidden_grad, total = pl.pallas_call(
        functools.partial(kernel, chunks),
        out_shape=(jax.ShapeDtypeStruct((rows, ff), BF), jax.ShapeDtypeStruct((depth, ff), BF)),
        in_specs=[any_spec] * 3,
        out_specs=(any_spec, any_spec),
        scratch_shapes=[
            pltpu.VMEM((2 * rows, 2 * depth), BF),
            pltpu.VMEM((2 * depth, 2 * rows), BF),
            block(2 * depth, BF),
            pltpu.VMEM((2, chunks, rows, fc), BF),
            block(rows, BF), block(rows, BF), block(rows, F32),
            block(depth, BF), block(depth, BF), block(depth, F32),
            block(depth, BF), block(depth, BF), block(depth, BF), block(depth, BF),
            block(rows, BF),
            sem, sem((chunks,)), sem((chunks,)), sem((chunks,)), sem((chunks,)),
            sem, sem, sem, sem,
        ] + [sem((chunks,))] * 14,
        compiler_params=pltpu.CompilerParams(
            collective_id=0, has_side_effects=True, vmem_limit_bytes=60 * 1024 * 1024
        ),
    )(hidden_pre, out_grad, down_weight)
    tokens_all = rows * lax.axis_size("rep") * lax.axis_size("fs")
    return hidden_grad, total.astype(F32) * (1.0 / math.sqrt(tokens_all))


def solution(mesh):
    placed = (P(("rep", "fs"), "tp"), P(("rep", "fs"), None), P("fs", "tp"))
    two_by_two = mesh.shape["fs"] == 4 and mesh.shape["tp"] == 2 and mesh.shape["rep"] == 4
    return jax.shard_map(
        paired_body if two_by_two else plain_body,
        mesh=mesh,
        in_specs=placed,
        out_specs=(P(("rep", "fs"), "tp"), P("fs", "tp")),
        check_vma=False,
    )
```

```python
import math

import jax
import jax.numpy as jnp
from jax import lax
from jax.experimental import pallas as pl
from jax.experimental.pallas import tpu as pltpu
from jax.sharding import PartitionSpec as P

MESH = pl.DeviceIdType.MESH
BF = jnp.bfloat16
F32 = jnp.float32


def plain_body(hidden_pre, out_grad, down_weight):
    rows = hidden_pre.shape[0]
    ff_local = hidden_pre.shape[1]
    back = jnp.dot(
        out_grad,
        lax.all_gather(down_weight, "fs", axis=0, tiled=True),
        preferred_element_type=F32,
    )
    positive = jnp.maximum(hidden_pre.astype(F32), 0.0)
    hidden_grad = (2.0 * positive * back).astype(BF)
    act = (positive * positive).astype(BF)
    partial_value = lax.dot_general(
        out_grad, act, (((0,), (0,)), ((), ())), preferred_element_type=F32
    )
    partial_value = partial_value.astype(BF)
    received = lax.all_to_all(partial_value, "fs", split_axis=0, concat_axis=0, tiled=True)
    groups = lax.axis_size("fs")
    local_sum = jnp.sum(
        received.reshape(groups, received.shape[0] // groups, ff_local), axis=0, dtype=F32
    )
    total = lax.psum(local_sum, "rep")
    tokens_all = rows * lax.axis_size("rep") * groups
    return (hidden_grad, total * (1.0 / math.sqrt(tokens_all)))


STEPS = 4


def kernel(hp, og, w, hg_out, tot_out,
           ogcat, ogt, whalf, hpc, pbs, pbr, pbo, gs, gr, gown, zs, z1r, z2r, zt, hg,
           l_og, l_w, l_hp, o_hg, o_t,
           og_s, og_r, od_s, od_r, w_s, w_r, f_s, f_r, hp_s, hp_r, pb_s, pb_r, g_s, g_r,
           z1_s, z1_rs, z2_s, z2_rs, z3_s, z3_rs):
    rows, ff = hp.shape
    depth = w.shape[0]
    chunks = 2 * STEPS
    fc = ff // chunks
    part = rows // 2
    fs = lax.axis_index("fs")
    core = lax.axis_index("tp")
    z = lax.axis_index("rep")
    last = lax.axis_size("rep") - 1
    a, b = fs // 2, fs % 2
    par = z % 2
    apeer = {"fs": (1 - a) * 2 + b}
    bpeer = {"fs": a * 2 + (1 - b)}
    cpeer = {"tp": 1 - core}
    znext = {"rep": z + 1 - 2 * par}
    zmid = {"rep": last - z}
    outer = jnp.logical_or(z == 0, z == last)
    inner = jnp.logical_not(outer)
    token_peer = (apeer, bpeer)
    weight_peer = (bpeer, apeer)

    def remote(src, dst, ssem, rsem, peer):
        return pltpu.make_async_remote_copy(
            src_ref=src, dst_ref=dst, send_sem=ssem, recv_sem=rsem,
            device_id=peer, device_id_type=MESH)

    def cut(i, size):
        return pl.ds(pl.multiple_of(i * size, size), size)

    place = (b, a)
    mine = [cut(place[q], depth) for q in range(2)]
    theirs = [cut(1 - place[q], depth) for q in range(2)]
    own_block = lambda q, p: 2 * a + p if q == 0 else 2 * p + b
    far_block = lambda q, p: 2 * (1 - a) + p if q == 0 else 2 * p + 1 - b
    low = cut(core, part)
    mid = pl.ds(pl.multiple_of(rows + core * part, part), part)
    mid_other = pl.ds(pl.multiple_of(rows + (1 - core) * part, part), part)
    both = [(q, p) for q in range(2) for p in range(2)]

    def load_og(q, p):
        return pltpu.make_async_copy(
            og.at[:, cut(own_block(q, p), depth)],
            ogcat.at[q, pl.ds(0, rows), pl.ds(p * depth, depth)], l_og.at[q, p])

    def load_w(c, q):
        return pltpu.make_async_copy(w.at[:, cut(c, fc)], whalf.at[c, mine[q]], l_w.at[c])

    def load_hp(c):
        return pltpu.make_async_copy(hp.at[:, cut(c, fc)], hpc.at[0, c], l_hp.at[c])

    def store_hg(c):
        return pltpu.make_async_copy(hg.at[c], hg_out.at[:, cut(c, fc)], o_hg.at[c])

    def store_tot(c):
        return pltpu.make_async_copy(zt.at[c], tot_out.at[:, cut(c, fc)], o_t.at[c])

    def send_og(q, p):
        return remote(og.at[low, cut(far_block(q, p), depth)],
                      ogcat.at[q, mid, pl.ds(p * depth, depth)],
                      og_s.at[q, p], og_r.at[q, p], token_peer[q])

    def pass_og(q, p, span):
        spot = ogcat.at[q, span, pl.ds(p * depth, depth)]
        return remote(spot, spot, od_s.at[q, p], od_r.at[q, p], cpeer)

    def send_w(c, q):
        return remote(w.at[:, cut(c, fc)], whalf.at[c, mine[q]], w_s.at[c], w_r.at[c], weight_peer[q])

    def recv_w(c, q):
        return remote(w.at[:, cut(c, fc)], whalf.at[c, theirs[q]], w_s.at[c], w_r.at[c], weight_peer[q])

    def pass_w(c, q):
        spot = whalf.at[c, theirs[q]]
        return remote(spot, spot, f_s.at[c], f_r.at[c], znext)

    def send_hp(c, q):
        return remote(hp.at[:, cut(c, fc)], hpc.at[1, c], hp_s.at[c], hp_r.at[c], token_peer[q])

    def send_pb(c, q):
        return remote(pbs.at[c], pbr.at[c], pb_s.at[c], pb_r.at[c], token_peer[q])

    def send_g(c, q):
        return remote(gs.at[c], gr.at[c], g_s.at[c], g_r.at[c], weight_peer[q])

    def send_z1(c):
        return remote(zs.at[c], z1r.at[c], z1_s.at[c], z1_rs.at[c], znext)

    def send_z2(c):
        return remote(zs.at[c], z2r.at[c], z2_s.at[c], z2_rs.at[c], zmid)

    def send_z3(c):
        return remote(zt.at[c], zt.at[c], z3_s.at[c], z3_rs.at[c], znext)

    def kept(j, q):
        return 2 * (2 * j + par) + q

    def passed(j, q):
        return 2 * (2 * j + 1 - par) + q

    def g_step(s):
        for q in range(2):
            c = 2 * s + q
            load_hp(c).wait()
            send_hp(c, q).wait_recv()
            if s + 2 < STEPS:
                send_hp(c + 4, q).start()
            positive = jnp.maximum(hpc[:, c].reshape(2 * rows, fc).astype(F32), 0.0)
            act = (positive * positive).astype(BF)
            gs[c] = jnp.dot(ogt[q, theirs[q], :], act, preferred_element_type=F32).astype(BF)
            send_g(c, q).start()
            gown[c] = jnp.dot(ogt[q, mine[q], :], act, preferred_element_type=F32)

    def z_a(s):
        for q in range(2):
            c = 2 * s + q
            send_g(c, q).wait_recv()

            @pl.when(outer)
            def _():
                zs[c] = (gown[c] + gr[c].astype(F32)).astype(BF)
                send_z1(c).start()

    def z_b(s):
        @pl.when(inner)
        def _():
            for q in range(2):
                c = 2 * s + q
                send_z1(c).wait_recv()
                zs[c] = (gown[c] + gr[c].astype(F32) + z1r[c].astype(F32)).astype(BF)
                send_z2(c).start()

    def z_c(s):
        @pl.when(inner)
        def _():
            for q in range(2):
                c = 2 * s + q
                send_z2(c).wait_recv()
                zt[c] = (zs[c].astype(F32) + z2r[c].astype(F32)).astype(BF)
                send_z3(c).start()
                store_tot(c).start()

    def z_d(s):
        @pl.when(outer)
        def _():
            for q in range(2):
                c = 2 * s + q
                send_z3(c).wait_recv()
                store_tot(c).start()

    def back(c, q):
        load_w(c, q).wait()
        pbs[c] = jnp.dot(ogcat[q, rows:2 * rows, :], whalf[c], preferred_element_type=F32).astype(BF)
        send_pb(c, q).start()
        pbo[c] = jnp.dot(ogcat[q, 0:rows, :], whalf[c], preferred_element_type=F32)

    def pb_direct(j):
        for which in (kept, passed):
            for q in range(2):
                recv_w(which(j, q), q).wait_recv()
                back(which(j, q), q)

    def pb_first():
        for q in range(2):
            back(kept(0, q), q)
        for q in range(2):
            pass_w(passed(0, q), q).wait_recv()
            back(passed(0, q), q)

    def finish(which, j):
        for q in range(2):
            c = which(j, q)
            send_pb(c, q).wait_recv()
            positive = jnp.maximum(hpc[0, c].astype(F32), 0.0)
            hg[c] = (2.0 * positive * (pbo[c] + pbr[c].astype(F32))).astype(BF)
            store_hg(c).start()

    barrier = pltpu.get_barrier_semaphore()
    for peer in (apeer, bpeer, cpeer, znext, zmid):
        pl.semaphore_signal(barrier, inc=1, device_id=peer, device_id_type=MESH)
    for q, p in both:
        load_og(q, p).start()
    pl.semaphore_wait(barrier, 5)
    for q, p in both:
        send_og(q, p).start()
    for q in range(2):
        send_w(kept(0, q), q).start()
    for s in range(2):
        for q in range(2):
            send_hp(2 * s + q, q).start()
    for c in range(chunks):
        load_hp(c).start()
    for c in range(chunks):
        load_w(c, c % 2).start()
    for q, p in both:
        load_og(q, p).wait()
    for q in range(2):
        ogt[q, :, 0:rows] = ogcat[q, 0:rows, :].T
    for p in range(2):
        for q in range(2):
            send_og(q, p).wait_recv()
            pass_og(q, p, mid).start()
    for q in range(2):
        for p in range(2):
            pass_og(q, p, mid_other).wait_recv()
        ogt[q, :, rows:2 * rows] = ogcat[q, rows:2 * rows, :].T

    for q in range(2):
        recv_w(kept(0, q), q).wait_recv()
        pass_w(kept(0, q), q).start()

    g_step(0)
    g_step(1)
    z_a(0)
    g_step(2)
    z_a(1)
    g_step(3)
    z_b(0)
    pb_first()
    z_a(2)
    for which in (kept, passed):
        for q in range(2):
            send_w(which(1, q), q).start()
    z_a(3)
    z_b(1)
    z_c(0)
    z_b(2)
    z_c(1)
    pb_direct(1)
    z_b(3)
    finish(kept, 0)
    finish(passed, 0)
    z_c(2)
    z_c(3)
    finish(kept, 1)
    z_d(0)
    z_d(1)
    z_d(2)
    z_d(3)
    finish(passed, 1)

    for q, p in both:
        send_og(q, p).wait_send()
        pass_og(q, p, mid).wait_send()
    for q in range(2):
        pass_w(kept(0, q), q).wait_send()
        for c in (kept(0, q), kept(1, q), passed(1, q)):
            send_w(c, q).wait_send()
    for c in range(chunks):
        send_hp(c, c % 2).wait_send()
        send_pb(c, c % 2).wait_send()
        send_g(c, c % 2).wait_send()
        store_hg(c).wait()
        store_tot(c).wait()

    @pl.when(outer)
    def _():
        for c in range(chunks):
            send_z1(c).wait_send()

    @pl.when(inner)
    def _():
        for c in range(chunks):
            send_z2(c).wait_send()
            send_z3(c).wait_send()


def paired_body(hidden_pre, out_grad, down_weight):
    rows, ff = hidden_pre.shape
    depth = down_weight.shape[0]
    chunks = 2 * STEPS
    fc = ff // chunks
    any_spec = pl.BlockSpec(memory_space=pl.ANY)

    def block(r, dtype):
        return pltpu.VMEM((chunks, r, fc), dtype)

    sem = pltpu.SemaphoreType.DMA
    hidden_grad, total = pl.pallas_call(
        kernel,
        out_shape=(jax.ShapeDtypeStruct((rows, ff), BF), jax.ShapeDtypeStruct((depth, ff), BF)),
        in_specs=[any_spec] * 3,
        out_specs=(any_spec, any_spec),
        scratch_shapes=[
            pltpu.VMEM((2, 2 * rows, 2 * depth), BF),
            pltpu.VMEM((2, 2 * depth, 2 * rows), BF),
            block(2 * depth, BF),
            pltpu.VMEM((2, chunks, rows, fc), BF),
            block(rows, BF), block(rows, BF), block(rows, F32),
            block(depth, BF), block(depth, BF), block(depth, F32),
            block(depth, BF), block(depth, BF), block(depth, BF), block(depth, BF),
            block(rows, BF),
            sem((2, 2)), sem((chunks,)), sem((chunks,)), sem((chunks,)), sem((chunks,)),
        ] + [sem((2, 2))] * 4 + [sem((chunks,))] * 16,
        compiler_params=pltpu.CompilerParams(
            collective_id=0, has_side_effects=True, vmem_limit_bytes=60 * 1024 * 1024
        ),
    )(hidden_pre, out_grad, down_weight)
    tokens_all = rows * lax.axis_size("rep") * lax.axis_size("fs")
    return hidden_grad, total.astype(F32) * (1.0 / math.sqrt(tokens_all))


def solution(mesh):
    placed = (P(("rep", "fs"), "tp"), P(("rep", "fs"), None), P("fs", "tp"))
    two_by_two = mesh.shape["fs"] == 4 and mesh.shape["tp"] == 2 and mesh.shape["rep"] == 4
    return jax.shard_map(
        paired_body if two_by_two else plain_body,
        mesh=mesh,
        in_specs=placed,
        out_specs=(P(("rep", "fs"), "tp"), P("fs", "tp")),
        check_vma=False,
    )
```
